32 devices in a mesh: ep: 8 (over z, core), tp: 4 (over y, x).
Axes of the slice: x: 2, y: 2, z: 4, core: 2. Of those that a mesh axis runs over, the one named last changes fastest.
Arguments:
- tokens: bfloat16 [512, 2048], P('ep'), may hold values from -6 to 6
- mix_gain: float32 [2048], replicated, may hold values from 0.1 to 1.9
- w_in: bfloat16 [2048, 1024], P(None, 'tp'), may hold values from -0.125 to 0.125
- decay_re: float32 [64, 64], P('tp'), may hold values from -1 to -0.1
- freq: float32 [64, 64], P('tp'), may hold values from 0 to 100
- log_step: float32 [64], P('tp'), may hold values from -3.9 to 0
- in_re: bfloat16 [64, 16, 64], P('tp'), may hold values from -1 to 1
- in_im: bfloat16 [64, 16, 64], P('tp'), may hold values from -1 to 1
- out_re: bfloat16 [64, 16, 64], P('tp'), may hold values from -0.75 to 0.75
- out_im: bfloat16 [64, 16, 64], P('tp'), may hold values from -0.75 to 0.75
- skip: float32 [64, 16], P('tp'), may hold values from -4 to 4
- state_re: float32 [512, 64, 64], P('ep', 'tp'), may hold values from -6 to 6
- state_im: float32 [512, 64, 64], P('ep', 'tp'), may hold values from -6 to 6
- glu_weight: bfloat16 [1024, 1024], P(None, 'tp'), may hold values from -0.1875 to 0.1875
- glu_bias: float32 [1024], P('tp'), may hold values from -4 to 4
- out_weight: bfloat16 [1024, 2048], P('tp'), may hold values from -0.1875 to 0.1875
- ffn_gain: float32 [2048], replicated, may hold values from 0.1 to 1.9
- route: int32 [512, 2], P('ep'), may hold values from 0 to 7, all different within a row; in each aligned block of 64 rows (0 to 63, 64 to 127, ...) at most 24 rows name the same one
- route_weight: float32 [512, 2], P('ep'), may hold values from 0.2 to 1
- expert_gate: bfloat16 [8, 2048, 3584], P('ep', None, 'tp'), may hold values from -0.125 to 0.125
- expert_up: bfloat16 [8, 2048, 3584], P('ep', None, 'tp'), may hold values from -0.125 to 0.125
- expert_down: bfloat16 [8, 3584, 2048], P('ep', 'tp'), may hold values from -0.09375 to 0.09375
Outputs:
- mixed: bfloat16 [512, 2048], P('ep', 'tp')
- new_re: float32 [512, 64, 64], P('ep', 'tp')
- new_im: float32 [512, 64, 64], P('ep', 'tp')
The draws below stay inside these ranges and needn't reach their ends.
Inputs may be any that keep to these rules, and one draw needn't show every extreme that they name: `route`: each row names 2 different experts. Within the 64 rows of one index of ep no expert is named more than 24 times, and in every draw some expert is named exactly 24 times by the rows of some index of ep.
All inputs are finite; a program needn't handle non-finite values.
Results may differ from the reference program's by a relative error of at most 0.015.
Values may be sent and summed in bfloat16 or wider, within the bound.
No kernel may reach another device: no remote copies, remote signals or barrier semaphores. Data moves between devices by JAX's collectives and lax.ppermute only.
A program may use at most 64 MiB of HBM per device.

```python
import math
import jax
import jax.numpy as jnp
import numpy as np
from jax import lax

D = 2048
C = 1024
H = 16
P_SIZE = 64
FFE = 3584
TOPK = 2
SEQ_GRP = 64
G = 64
EXPERTS = 8
SEQS = 512
CAP = 24
ROWS_E = 192
N_TP = 4


def levels(rng, shape, pieces, low, largest):
    def one(dim, blocks):
        heights = jax.random.uniform(jax.random.fold_in(jax.random.fold_in(rng, 6), dim), (blocks,), jnp.float32, low / len(pieces), largest / len(pieces))
        return jnp.repeat(jnp.exp(heights), shape[dim] // blocks).reshape((-1,) + (1,) * (len(shape) - dim - 1))

    level = one(*pieces[0])
    for cut in pieces[1:]:
        level = level * one(*cut)
    return level


def routed_block(key, own, number, rows, count, top, bound, lean):
    ranking = jax.random.permutation(key, count)
    crowded, usual = portions_of(count, rows * top, bound, lean, True), portions_of(count, rows * top, bound, lean, False)
    places = jnp.arange(count)

    def named(tallies, turn):
        used = int((tallies > 0).sum())
        fixed = max(1, used // 4)
        moved = fixed + (places - fixed + turn * (used - fixed)) % max(1, count - fixed)
        return jnp.zeros((count,), jnp.int32).at[ranking[jnp.where(places < fixed, places, moved)]].set(jnp.asarray(tallies, jnp.int32))

    tallies = jnp.where(number % 4 == 0, named(crowded, number // 4), named(usual, number - number // 4 - 1))
    mixed = jax.random.permutation(jax.random.fold_in(own, 3), count)
    donor, taker = mixed[0:count // 2 * 2:2], mixed[1:count // 2 * 2:2]
    margin = jnp.minimum(tallies[donor] - 1, bound - tallies[taker]) // 2
    margin = jnp.where((donor == ranking[0]) | (taker == ranking[0]) | (tallies[taker] == 0), 0, jnp.maximum(margin, 0))
    moved = jax.random.randint(jax.random.fold_in(own, 4), (count // 2,), 0, 1 << 20) % (margin + 1)
    tallies = tallies.at[donor].add(-moved).at[taker].add(moved)
    members = jnp.searchsorted(jnp.cumsum(tallies), jnp.arange(rows * top), side="right").astype(jnp.int32)
    listing = members.reshape(top, rows).T
    listing = listing[jax.random.permutation(jax.random.fold_in(own, 1), rows)]
    turn = jax.random.randint(jax.random.fold_in(own, 2), (rows, 1), 0, top)
    return jnp.take_along_axis(listing, (jnp.arange(top)[None, :] + turn) % top, axis=1)


def portions_of(amount, total, bound, slope, full):
    loads = [(1 << 20) // math.isqrt(rank ** slope) + 1 for rank in range(1, amount + 1)]
    largest = bound if full else min(bound, max(-(-total // amount), total * loads[0] // sum(loads)))
    least = 1 if total - largest >= amount - 1 else 0
    holding, spare = [largest] + [least] * (amount - 1), total - largest - least * (amount - 1)
    while spare > 0:
        candidates = [i for i in range(1, amount) if holding[i] < largest] or [i for i in range(1, amount) if holding[i] < bound]
        whole, budget = sum([loads[i] for i in candidates]), spare
        for i in candidates:
            addition = min(bound - holding[i], max(1, budget * loads[i] // whole), spare)
            holding[i] = holding[i] + addition
            spare = spare - addition
    return np.array(holding)


def bell_draw(rng, shape, spread, most, split=(), kind=jnp.bfloat16):
    level = levels(rng, shape, split, -0.22, 0.18) if split else 1.0
    entries = jax.random.normal(rng, shape, jnp.float32) * spread * level
    return jnp.minimum(jnp.maximum(entries, -most), most).astype(kind)


def setup_inputs(seed: int = 0) -> dict:
    splits = jax.random.split(jax.random.key(seed), 23)
    tokens = bell_draw(splits[0], (SEQS, D), 1.0, 6.0, ((0, 8),))
    mix_gain = jnp.clip(1.0 + 0.18 * jax.random.normal(splits[1], (D,), jnp.float32), 0.1, 1.9)
    w_in = bell_draw(splits[2], (D, C), D ** -0.5, 0.125, ((1, 4),))
    decay_re = jnp.clip(-1.0 + 0.9 * jax.random.uniform(splits[3], (G, P_SIZE), jnp.float32) ** levels(splits[3], (G, P_SIZE), ((0, 4),), -0.2, 0.2), -1.0, -0.1)
    freq = jnp.clip(100.0 * jax.random.uniform(splits[4], (G, P_SIZE), jnp.float32) ** levels(splits[4], (G, P_SIZE), ((0, 4),), -0.2, 0.2), 0.0, 100.0)
    log_step = jnp.clip(-3.9 + 3.9 * jax.random.uniform(splits[5], (G,), jnp.float32) ** levels(splits[5], (G,), ((0, 4),), -0.2, 0.2), -3.9, 0.0)
    in_re = bell_draw(splits[6], (G, H, P_SIZE), (2 * H) ** -0.5, 1.0, ((0, 4),))
    in_im = bell_draw(splits[7], (G, H, P_SIZE), (2 * H) ** -0.5, 1.0, ((0, 4),))
    out_re = bell_draw(splits[8], (G, H, P_SIZE), P_SIZE ** -0.5, 0.75, ((0, 4),))
    out_im = bell_draw(splits[9], (G, H, P_SIZE), P_SIZE ** -0.5, 0.75, ((0, 4),))
    skip = bell_draw(splits[10], (G, H), 1.0, 4.0, ((0, 4),), jnp.float32)
    state_re = bell_draw(splits[11], (SEQS, G, P_SIZE), 1.0, 6.0, ((0, 8), (1, 4)), jnp.float32)
    state_im = bell_draw(splits[12], (SEQS, G, P_SIZE), 1.0, 6.0, ((0, 8), (1, 4)), jnp.float32)
    glu_weight = bell_draw(splits[13], (C, C), C ** -0.5, 0.1875, ((1, 4),))
    glu_bias = bell_draw(splits[14], (C,), 1.0, 4.0, ((0, 4),), jnp.float32)
    out_weight = bell_draw(splits[15], (C, D), C ** -0.5, 0.1875, ((0, 4),))
    ffn_gain = jnp.clip(1.0 + 0.18 * jax.random.normal(splits[16], (D,), jnp.float32), 0.1, 1.9)
    route_keys = jax.random.split(jax.random.fold_in(splits[17], 1), SEQS // SEQ_GRP)
    route_turns = jax.random.permutation(jax.random.fold_in(splits[17], 3), SEQS // SEQ_GRP)
    route = jax.vmap(lambda own, number: routed_block(jax.random.fold_in(splits[17], 2), own, number, SEQ_GRP, EXPERTS, TOPK, CAP, 2))(route_keys, route_turns).reshape((SEQS, TOPK))
    route_weight = jnp.clip(0.2 + 0.8 * jax.random.uniform(splits[18], (SEQS, TOPK), jnp.float32) ** levels(splits[18], (SEQS, TOPK), ((0, 8),), -0.2, 0.2), 0.2, 1.0)
    expert_gate = bell_draw(splits[19], (EXPERTS, D, FFE), D ** -0.5, 0.125, ((0, 8), (2, 4)))
    expert_up = bell_draw(splits[20], (EXPERTS, D, FFE), D ** -0.5, 0.125, ((0, 8), (2, 4)))
    expert_down = bell_draw(splits[21], (EXPERTS, FFE, D), FFE ** -0.5, 0.09375, ((0, 8), (1, 4)))
    return {"tokens": tokens, "mix_gain": mix_gain, "w_in": w_in, "decay_re": decay_re, "freq": freq, "log_step": log_step, "in_re": in_re, "in_im": in_im, "out_re": out_re, "out_im": out_im, "skip": skip, "state_re": state_re, "state_im": state_im, "glu_weight": glu_weight, "glu_bias": glu_bias, "out_weight": out_weight, "ffn_gain": ffn_gain, "route": route, "route_weight": route_weight, "expert_gate": expert_gate, "expert_up": expert_up, "expert_down": expert_down}


norm_eps = 1e-06

def rms_scale(rows, gain):
    values = rows.astype(jnp.float32)
    scaled = values * lax.rsqrt(lax.optimization_barrier(jnp.mean(values * values, axis=-1, keepdims=True)) + norm_eps)
    return (scaled * gain).astype(jnp.bfloat16)

def split_sum(left, right, parts):
    width = left.shape[1] // parts
    lefts = jnp.moveaxis(left.reshape(left.shape[0], parts, width), 1, 0)
    rights = right.reshape(parts, width, right.shape[1])

    def add_block(total, pair):
        term = jnp.dot(pair[0], pair[1], preferred_element_type=jnp.float32).astype(jnp.bfloat16)
        term = lax.optimization_barrier(term)
        return (total + term.astype(jnp.float32), None)
    start = jnp.zeros((left.shape[0], right.shape[1]), jnp.float32)
    total, _ = lax.scan(add_block, start, (lefts, rights))
    return total

def state_step(inputs, state_re, state_im, decay_re, freq, log_step, in_re, in_im, out_re, out_im, skip):
    highest = lax.Precision.HIGHEST
    step = jnp.exp(log_step)[:, None]
    magnitude = jnp.exp(decay_re * step)
    turn_re = magnitude * jnp.cos(freq * step)
    turn_im = magnitude * jnp.sin(freq * step)
    denom = decay_re * decay_re + freq * freq
    coef_re = ((turn_re - 1.0) * decay_re + turn_im * freq) / denom
    coef_im = (turn_im * decay_re - (turn_re - 1.0) * freq) / denom
    values = inputs.astype(jnp.float32)
    drive_re = jnp.einsum('sgh,ghp->sgp', values, in_re.astype(jnp.float32), precision=highest)
    drive_im = jnp.einsum('sgh,ghp->sgp', values, in_im.astype(jnp.float32), precision=highest)
    push_re = coef_re * drive_re - coef_im * drive_im
    push_im = coef_re * drive_im + coef_im * drive_re
    new_re = turn_re * state_re - turn_im * state_im + push_re
    new_im = turn_re * state_im + turn_im * state_re + push_im
    read = jnp.einsum('ghp,sgp->sgh', out_re.astype(jnp.float32), new_re, precision=highest)
    read = read - jnp.einsum('ghp,sgp->sgh', out_im.astype(jnp.float32), new_im, precision=highest)
    read = read + skip * values
    return (read, new_re, new_im)

def reference(tokens, mix_gain, w_in, decay_re, freq, log_step, in_re, in_im, out_re, out_im, skip, state_re, state_im, glu_weight, glu_bias, out_weight, ffn_gain, route, route_weight, expert_gate, expert_up, expert_down):
    normed = rms_scale(tokens, mix_gain)
    drive = jnp.dot(normed, w_in, preferred_element_type=jnp.float32).astype(jnp.bfloat16)
    inputs = drive.reshape(SEQS, G, H)
    read, new_re, new_im = state_step(inputs, state_re, state_im, decay_re, freq, log_step, in_re, in_im, out_re, out_im, skip)
    mixed_in = jax.nn.gelu(read).reshape(SEQS, C).astype(jnp.bfloat16)
    gate = jnp.dot(mixed_in, glu_weight, preferred_element_type=jnp.float32) + glu_bias
    gated = (mixed_in.astype(jnp.float32) * jax.nn.sigmoid(gate)).astype(jnp.bfloat16)
    mix_total = split_sum(gated, out_weight, N_TP)
    resid = (tokens.astype(jnp.float32) + mix_total).astype(jnp.bfloat16)
    normed2 = rms_scale(resid, ffn_gain)
    flat_route = route.reshape(-1)
    flat_weight = route_weight.reshape(-1)

    def expert_pass(total, inputs_e):
        gate_w, up_w, down_w, index = inputs_e
        hits = flat_route == index
        picked = jnp.nonzero(hits, size=ROWS_E, fill_value=0)[0].astype(jnp.int32)
        valid = (jnp.arange(ROWS_E) < jnp.sum(hits.astype(jnp.int32))).astype(jnp.float32)
        token_ids = (picked // TOPK).astype(jnp.int32)
        rows = normed2[token_ids]
        gate_e = jnp.dot(rows, gate_w, preferred_element_type=jnp.float32)
        up_e = jnp.dot(rows, up_w, preferred_element_type=jnp.float32)
        hidden = (jax.nn.silu(gate_e) * up_e).astype(jnp.bfloat16)
        result = split_sum(hidden, down_w, N_TP).astype(jnp.bfloat16)
        weight = flat_weight[picked] * valid
        total = total.at[token_ids].add(weight[:, None] * result.astype(jnp.float32))
        return (total, None)
    start = resid.astype(jnp.float32)
    indices = jnp.arange(EXPERTS).astype(jnp.int32)
    total, _ = lax.scan(expert_pass, start, (expert_gate, expert_up, expert_down, indices))
    return (total.astype(jnp.bfloat16), new_re, new_im)
```

```python
import jax
import jax.numpy as jnp
from jax import lax
from jax.sharding import PartitionSpec as P

norm_eps = 1e-06


def rms_scale(rows, gain):
    values = rows.astype(jnp.float32)
    scaled = values * lax.rsqrt(jnp.mean(values * values, axis=-1, keepdims=True) + norm_eps)
    return (scaled * gain).astype(jnp.bfloat16)


def state_step(
    inputs, state_re, state_im, decay_re, freq, log_step, in_re, in_im, out_re, out_im, skip
):
    highest = lax.Precision.HIGHEST
    step = jnp.exp(log_step)[:, None]
    magnitude = jnp.exp(decay_re * step)
    turn_re = magnitude * jnp.cos(freq * step)
    turn_im = magnitude * jnp.sin(freq * step)
    denom = decay_re * decay_re + freq * freq
    coef_re = ((turn_re - 1.0) * decay_re + turn_im * freq) / denom
    coef_im = (turn_im * decay_re - (turn_re - 1.0) * freq) / denom
    drive_re = jnp.einsum("sgh,ghp->sgp", inputs, in_re, preferred_element_type=jnp.float32)
    drive_im = jnp.einsum("sgh,ghp->sgp", inputs, in_im, preferred_element_type=jnp.float32)
    push_re = coef_re * drive_re - coef_im * drive_im
    push_im = coef_re * drive_im + coef_im * drive_re
    new_re = turn_re * state_re - turn_im * state_im + push_re
    new_im = turn_re * state_im + turn_im * state_re + push_im
    read = jnp.einsum("ghp,sgp->sgh", out_re.astype(jnp.float32), new_re, precision=highest)
    read = read - jnp.einsum("ghp,sgp->sgh", out_im.astype(jnp.float32), new_im, precision=highest)
    read = read + skip * inputs.astype(jnp.float32)
    return (read, new_re, new_im)


def partner_swap(value, offset):
    count = lax.axis_size("tp")
    return lax.ppermute(value, "tp", [(source, source ^ offset) for source in range(count)])


def local(
    tokens,
    mix_gain,
    w_in,
    decay_re,
    freq,
    log_step,
    in_re,
    in_im,
    out_re,
    out_im,
    skip,
    state_re,
    state_im,
    glu_weight,
    glu_bias,
    out_weight,
    ffn_gain,
    route,
    route_weight,
    expert_gate,
    expert_up,
    expert_down,
):
    seq_count = tokens.shape[0]
    groups_local = decay_re.shape[0]
    model_width = tokens.shape[1]
    shards = lax.axis_size("tp")
    local_width = model_width // shards
    experts = lax.axis_size("ep")
    top_count = route.shape[1]
    slot_cap = (3 * seq_count * top_count + 2 * experts - 1) // (2 * experts)
    rows_all = experts * slot_cap
    own = lax.axis_index("tp")
    offsets = list(range(1, shards))
    gate_local = expert_gate[0]
    up_local = expert_up[0]
    down_local = expert_down[0]

    def rows_of(array, offset, width):
        return lax.dynamic_slice_in_dim(array, (own ^ offset) * width, width, 0)

    def cols_of(array, offset, width):
        return lax.dynamic_slice_in_dim(array, (own ^ offset) * width, width, 1)

    normed = rms_scale(tokens, mix_gain)
    drive = jnp.dot(normed, w_in, preferred_element_type=jnp.float32).astype(jnp.bfloat16)
    inputs = drive.reshape(seq_count, groups_local, -1)
    read, new_re, new_im = state_step(
        inputs, state_re, state_im, decay_re, freq, log_step, in_re, in_im, out_re, out_im, skip
    )
    mixed_in = jax.nn.gelu(read).reshape(seq_count, -1).astype(jnp.bfloat16)
    chan_width = mixed_in.shape[1]

    arrived_mix = [partner_swap(mixed_in, offset) for offset in offsets]
    gate = jnp.dot(
        mixed_in, rows_of(glu_weight, 0, chan_width), preferred_element_type=jnp.float32
    )
    for offset, block in zip(offsets, arrived_mix):
        gate = gate + jnp.dot(
            block, rows_of(glu_weight, offset, chan_width), preferred_element_type=jnp.float32
        )
    gated = (mixed_in.astype(jnp.float32) * jax.nn.sigmoid(gate + glu_bias)).astype(jnp.bfloat16)

    def share(offset):
        block = jnp.dot(
            gated, cols_of(out_weight, offset, local_width), preferred_element_type=jnp.float32
        )
        return block.astype(jnp.bfloat16)

    arrived_shares = [partner_swap(share(offset), offset) for offset in offsets]
    mix_part = share(0).astype(jnp.float32)
    for block in arrived_shares:
        mix_part = mix_part + block.astype(jnp.float32)
    resid_part = (cols_of(tokens, 0, local_width).astype(jnp.float32) + mix_part).astype(
        jnp.bfloat16
    )

    flat_route = route.reshape(-1)
    hits = (flat_route[:, None] == jnp.arange(experts)[None, :]).astype(jnp.int32)
    rank = jnp.sum((jnp.cumsum(hits, axis=0) - hits) * hits, axis=1)
    slot = flat_route * slot_cap + rank
    slot_ids = jnp.arange(rows_all)
    picks = (slot[None, :] == slot_ids[:, None]).reshape(rows_all, seq_count, top_count)
    select = jnp.any(picks, axis=2).astype(jnp.bfloat16)
    combine = jnp.einsum("ask,sk->sa", picks.astype(jnp.float32), route_weight)

    outbound = jnp.dot(select, resid_part, preferred_element_type=jnp.float32).astype(jnp.bfloat16)
    arrived = lax.all_to_all(
        outbound.reshape(experts, slot_cap, local_width),
        "ep",
        split_axis=0,
        concat_axis=0,
        tiled=True,
    ).reshape(rows_all, local_width)
    blocks = [(0, arrived)] + [(offset, partner_swap(arrived, offset)) for offset in offsets]
    gate_rows = up_rows = squares = 0.0
    for offset, block in blocks:
        values = block.astype(jnp.float32)
        squares = squares + jnp.sum(values * values, axis=1, keepdims=True)
        gain = lax.dynamic_slice_in_dim(ffn_gain, (own ^ offset) * local_width, local_width, 0)
        scaled = (values * gain).astype(jnp.bfloat16)
        gate_rows = gate_rows + jnp.dot(
            scaled, rows_of(gate_local, offset, local_width), preferred_element_type=jnp.float32
        )
        up_rows = up_rows + jnp.dot(
            scaled, rows_of(up_local, offset, local_width), preferred_element_type=jnp.float32
        )
    row_scale = lax.rsqrt(squares / model_width + norm_eps)
    hidden = (jax.nn.silu(gate_rows * row_scale) * (up_rows * row_scale)).astype(jnp.bfloat16)

    def result(offset):
        block = jnp.dot(
            hidden, cols_of(down_local, offset, local_width), preferred_element_type=jnp.float32
        )
        return block.astype(jnp.bfloat16)

    arrived_results = [partner_swap(result(offset), offset) for offset in offsets]
    back_rows = result(0).astype(jnp.float32)
    for block in arrived_results:
        back_rows = back_rows + block.astype(jnp.float32)
    returned = lax.all_to_all(
        back_rows.astype(jnp.bfloat16).reshape(experts, slot_cap, local_width),
        "ep",
        split_axis=0,
        concat_axis=0,
        tiled=True,
    ).reshape(rows_all, local_width)
    expert_total = lax.dot_general(
        combine,
        returned.astype(jnp.float32),
        (((1,), (0,)), ((), ())),
        precision=lax.Precision.HIGHEST,
    )
    mixed = (resid_part.astype(jnp.float32) + expert_total).astype(jnp.bfloat16)
    return (mixed, new_re, new_im)


def solution(mesh):
    in_specs = (
        P("ep", None),
        P(),
        P(None, "tp"),
        P("tp", None),
        P("tp", None),
        P("tp"),
        P("tp", None, None),
        P("tp", None, None),
        P("tp", None, None),
        P("tp", None, None),
        P("tp", None),
        P("ep", "tp", None),
        P("ep", "tp", None),
        P(None, "tp"),
        P("tp"),
        P("tp", None),
        P(),
        P("ep", None),
        P("ep", None),
        P("ep", None, "tp"),
        P("ep", None, "tp"),
        P("ep", "tp", None),
    )
    out_specs = (P("ep", "tp"), P("ep", "tp", None), P("ep", "tp", None))
    return jax.shard_map(local, mesh=mesh, in_specs=in_specs, out_specs=out_specs, check_vma=False)
```

```python
import jax
import jax.numpy as jnp
from jax import lax
from jax.sharding import PartitionSpec as P

norm_eps = 1e-06


def rms_scale(rows, gain):
    values = rows.astype(jnp.float32)
    scaled = values * lax.rsqrt(jnp.mean(values * values, axis=-1, keepdims=True) + norm_eps)
    return (scaled * gain).astype(jnp.bfloat16)


def state_step(
    inputs, state_re, state_im, decay_re, freq, log_step, in_re, in_im, out_re, out_im, skip
):
    highest = lax.Precision.HIGHEST
    step = jnp.exp(log_step)[:, None]
    magnitude = jnp.exp(decay_re * step)
    turn_re = magnitude * jnp.cos(freq * step)
    turn_im = magnitude * jnp.sin(freq * step)
    denom = decay_re * decay_re + freq * freq
    coef_re = ((turn_re - 1.0) * decay_re + turn_im * freq) / denom
    coef_im = (turn_im * decay_re - (turn_re - 1.0) * freq) / denom
    drive_re = jnp.einsum("sgh,ghp->sgp", inputs, in_re, preferred_element_type=jnp.float32)
    drive_im = jnp.einsum("sgh,ghp->sgp", inputs, in_im, preferred_element_type=jnp.float32)
    push_re = coef_re * drive_re - coef_im * drive_im
    push_im = coef_re * drive_im + coef_im * drive_re
    new_re = turn_re * state_re - turn_im * state_im + push_re
    new_im = turn_re * state_im + turn_im * state_re + push_im
    read = jnp.einsum("ghp,sgp->sgh", out_re.astype(jnp.float32), new_re, precision=highest)
    read = read - jnp.einsum("ghp,sgp->sgh", out_im.astype(jnp.float32), new_im, precision=highest)
    read = read + skip * inputs.astype(jnp.float32)
    return (read, new_re, new_im)


def partner_swap(value, offset):
    count = lax.axis_size("tp")
    return lax.ppermute(value, "tp", [(source, source ^ offset) for source in range(count)])


def ep_swap(value, offset):
    count = lax.axis_size("ep")
    return lax.ppermute(value, "ep", [(source, source ^ offset) for source in range(count)])


def to_experts(rows):
    pairs = rows.shape[1]
    near = rows[0]
    crossed = ep_swap(rows[1], 1)
    joined = jnp.stack([near, crossed], axis=1)
    moved = [None] + [ep_swap(joined[step], 2 * step) for step in range(pairs - 1, 0, -1)][::-1]
    moved[0] = joined[0]
    return jnp.stack(moved, axis=0)


def from_experts(rows):
    pairs = rows.shape[0]
    moved = [None] + [ep_swap(rows[step], 2 * step) for step in range(pairs - 1, 0, -1)][::-1]
    moved[0] = rows[0]
    moved = jnp.stack(moved, axis=1)
    return jnp.stack([moved[0], ep_swap(moved[1], 1)], axis=0)


def local(
    tokens,
    mix_gain,
    w_in,
    decay_re,
    freq,
    log_step,
    in_re,
    in_im,
    out_re,
    out_im,
    skip,
    state_re,
    state_im,
    glu_weight,
    glu_bias,
    out_weight,
    ffn_gain,
    route,
    route_weight,
    expert_gate,
    expert_up,
    expert_down,
):
    seq_count = tokens.shape[0]
    groups_local = decay_re.shape[0]
    model_width = tokens.shape[1]
    shards = lax.axis_size("tp")
    local_width = model_width // shards
    experts = lax.axis_size("ep")
    top_count = route.shape[1]
    slot_cap = (3 * seq_count * top_count + 2 * experts - 1) // (2 * experts)
    rows_all = experts * slot_cap
    own = lax.axis_index("tp")
    offsets = list(range(1, shards))
    gate_local = expert_gate[0]
    up_local = expert_up[0]
    down_local = expert_down[0]

    def rows_of(array, offset, width):
        return lax.dynamic_slice_in_dim(array, (own ^ offset) * width, width, 0)

    def cols_of(array, offset, width):
        return lax.dynamic_slice_in_dim(array, (own ^ offset) * width, width, 1)

    normed = rms_scale(tokens, mix_gain)
    drive = jnp.dot(normed, w_in, preferred_element_type=jnp.float32).astype(jnp.bfloat16)
    inputs = drive.reshape(seq_count, groups_local, -1)
    read, new_re, new_im = state_step(
        inputs, state_re, state_im, decay_re, freq, log_step, in_re, in_im, out_re, out_im, skip
    )
    mixed_in = jax.nn.gelu(read).reshape(seq_count, -1).astype(jnp.bfloat16)
    chan_width = mixed_in.shape[1]

    arrived_mix = [partner_swap(mixed_in, offset) for offset in offsets]
    gate = jnp.dot(
        mixed_in, rows_of(glu_weight, 0, chan_width), preferred_element_type=jnp.float32
    )
    for offset, block in zip(offsets, arrived_mix):
        gate = gate + jnp.dot(
            block, rows_of(glu_weight, offset, chan_width), preferred_element_type=jnp.float32
        )
    gated = (mixed_in.astype(jnp.float32) * jax.nn.sigmoid(gate + glu_bias)).astype(jnp.bfloat16)

    def share(offset):
        block = jnp.dot(
            gated, cols_of(out_weight, offset, local_width), preferred_element_type=jnp.float32
        )
        return block.astype(jnp.bfloat16)

    arrived_shares = [partner_swap(share(offset), offset) for offset in offsets]
    mix_part = share(0).astype(jnp.float32)
    for block in arrived_shares:
        mix_part = mix_part + block.astype(jnp.float32)
    resid_part = (cols_of(tokens, 0, local_width).astype(jnp.float32) + mix_part).astype(
        jnp.bfloat16
    )

    flat_route = route.reshape(-1)
    hits = (flat_route[:, None] == jnp.arange(experts)[None, :]).astype(jnp.int32)
    rank = jnp.sum((jnp.cumsum(hits, axis=0) - hits) * hits, axis=1)
    relative = flat_route ^ lax.axis_index("ep")
    pairs = experts // 2
    slot = ((relative % 2) * pairs + relative // 2) * slot_cap + rank
    slot_ids = jnp.arange(rows_all)
    picks = (slot[None, :] == slot_ids[:, None]).reshape(rows_all, seq_count, top_count)
    select = jnp.any(picks, axis=2).astype(jnp.bfloat16)
    combine = jnp.einsum("ask,sk->sa", picks.astype(jnp.float32), route_weight)

    outbound = jnp.dot(select, resid_part, preferred_element_type=jnp.float32).astype(jnp.bfloat16)
    arrived = to_experts(outbound.reshape(2, pairs, slot_cap, local_width))
    arrived = arrived.reshape(rows_all, local_width)
    blocks = [(0, arrived)] + [(offset, partner_swap(arrived, offset)) for offset in offsets]
    gate_rows = up_rows = squares = 0.0
    for offset, block in blocks:
        values = block.astype(jnp.float32)
        squares = squares + jnp.sum(values * values, axis=1, keepdims=True)
        gain = lax.dynamic_slice_in_dim(ffn_gain, (own ^ offset) * local_width, local_width, 0)
        scaled = (values * gain).astype(jnp.bfloat16)
        gate_rows = gate_rows + jnp.dot(
            scaled, rows_of(gate_local, offset, local_width), preferred_element_type=jnp.float32
        )
        up_rows = up_rows + jnp.dot(
            scaled, rows_of(up_local, offset, local_width), preferred_element_type=jnp.float32
        )
    row_scale = lax.rsqrt(squares / model_width + norm_eps)
    hidden = (jax.nn.silu(gate_rows * row_scale) * (up_rows * row_scale)).astype(jnp.bfloat16)

    def result(offset):
        block = jnp.dot(
            hidden, cols_of(down_local, offset, local_width), preferred_element_type=jnp.float32
        )
        return block.astype(jnp.bfloat16)

    arrived_results = [partner_swap(result(offset), offset) for offset in offsets]
    back_rows = result(0).astype(jnp.float32)
    for block in arrived_results:
        back_rows = back_rows + block.astype(jnp.float32)
    returned = from_experts(
        back_rows.astype(jnp.bfloat16).reshape(pairs, 2, slot_cap, local_width)
    ).reshape(rows_all, local_width)
    expert_total = lax.dot_general(
        combine,
        returned.astype(jnp.float32),
        (((1,), (0,)), ((), ())),
        precision=lax.Precision.HIGHEST,
    )
    mixed = (resid_part.astype(jnp.float32) + expert_total).astype(jnp.bfloat16)
    return (mixed, new_re, new_im)


def solution(mesh):
    in_specs = (
        P("ep", None),
        P(),
        P(None, "tp"),
        P("tp", None),
        P("tp", None),
        P("tp"),
        P("tp", None, None),
        P("tp", None, None),
        P("tp", None, None),
        P("tp", None, None),
        P("tp", None),
        P("ep", "tp", None),
        P("ep", "tp", None),
        P(None, "tp"),
        P("tp"),
        P("tp", None),
        P(),
        P("ep", None),
        P("ep", None),
        P("ep", None, "tp"),
        P("ep", None, "tp"),
        P("ep", "tp", None),
    )
    out_specs = (P("ep", "tp"), P("ep", "tp", None), P("ep", "tp", None))
    return jax.shard_map(local, mesh=mesh, in_specs=in_specs, out_specs=out_specs, check_vma=False)
```

```python
import functools

import jax
import jax.numpy as jnp
from jax import lax
from jax.experimental import pallas as pl
from jax.experimental.pallas import tpu as pltpu
from jax.sharding import PartitionSpec as P

norm_eps = 1e-06


def partner_swap(value, offset):
    count = lax.axis_size("tp")
    return lax.ppermute(value, "tp", [(source, source ^ offset) for source in range(count)])


def ep_swap(value, offset):
    count = lax.axis_size("ep")
    return lax.ppermute(value, "ep", [(source, source ^ offset) for source in range(count)])


def to_experts(rows):
    pairs = rows.shape[1]
    near = rows[0]
    crossed = ep_swap(rows[1], 1)
    joined = jnp.stack([near, crossed], axis=1)
    moved = [None] + [ep_swap(joined[step], 2 * step) for step in range(pairs - 1, 0, -1)][::-1]
    moved[0] = joined[0]
    return jnp.stack(moved, axis=0), joined


def from_experts(rows):
    pairs = rows.shape[0]
    moved = [None] + [ep_swap(rows[step], 2 * step) for step in range(pairs - 1, 0, -1)][::-1]
    moved[0] = rows[0]
    moved = jnp.stack(moved, axis=1)
    return jnp.stack([moved[0], ep_swap(moved[1], 1)], axis=0)


def lane_sums(values):
    total = values[:, :128]
    for start in range(128, values.shape[1], 128):
        total = total + values[:, start : start + 128]
    return total


def mixer_front(
    at_ref,
    gain_ref,
    log_step_ref,
    decay_ref,
    freq_ref,
    in_re_ref,
    in_im_ref,
    out_re_ref,
    out_im_ref,
    skip_ref,
    tokens_hbm,
    w_in_hbm,
    state_re_hbm,
    state_im_hbm,
    mixed_ref,
    kept_ref,
    new_re_ref,
    new_im_ref,
    tokens_ref,
    w_in_ref,
    state_re_ref,
    state_im_ref,
    in_ref,
    out_ref,
    split_ref,
    sems,
):
    groups, heads, entries = in_re_ref.shape
    seqs, width = tokens_ref.shape
    per_half = min(groups, max(1, 128 // heads))
    lanes = 2 * entries
    copies = [
        pltpu.make_async_copy(source, target, sems.at[place])
        for place, (source, target) in enumerate(
            (
                (tokens_hbm, tokens_ref),
                (w_in_hbm, w_in_ref),
                (state_re_hbm, state_re_ref),
                (state_im_hbm, state_im_ref),
            )
        )
    ]
    for copy in copies:
        copy.start()

    in_ref[...] = jnp.zeros_like(in_ref)
    out_ref[...] = jnp.zeros_like(out_ref)
    for g in range(groups):
        rows = pl.ds((g % per_half) * heads, heads)
        in_ref[rows, g * lanes : (g + 1) * lanes] = jnp.concatenate(
            [in_re_ref[g], in_im_ref[g]], axis=1
        )
        out_ref[rows, g * lanes : (g + 1) * lanes] = jnp.concatenate(
            [out_re_ref[g], -out_im_ref[g]], axis=1
        )

    diagonal = lax.broadcasted_iota(jnp.int32, (groups, groups), 0) == lax.broadcasted_iota(
        jnp.int32, (groups, groups), 1
    )
    step = jnp.sum(
        jnp.where(diagonal, jnp.exp(log_step_ref[...]), 0.0), axis=1, keepdims=True
    )
    decay, freq = decay_ref[...], freq_ref[...]
    magnitude = jnp.exp(decay * step)
    turn_re = magnitude * jnp.cos(freq * step)
    turn_im = magnitude * jnp.sin(freq * step)
    denom = decay * decay + freq * freq
    coef_re = ((turn_re - 1.0) * decay + turn_im * freq) / denom
    coef_im = (turn_im * decay - (turn_re - 1.0) * freq) / denom

    block = per_half * heads
    skip_tiled = jnp.concatenate([skip_ref[...]] * per_half, axis=1)
    owner = lax.broadcasted_iota(jnp.int32, skip_tiled.shape, 1) // heads
    group = lax.broadcasted_iota(jnp.int32, skip_tiled.shape, 0)
    skip_rows = [
        jnp.sum(jnp.where(owner + start == group, skip_tiled, 0.0), axis=0, keepdims=True)
        for start in range(0, groups, per_half)
    ]

    copies[0].wait()
    values = tokens_ref[...].astype(jnp.float32)
    squares = jnp.sum(lane_sums(values * values), axis=1, keepdims=True)
    scale = lax.rsqrt(squares / width + norm_eps)
    normed = (values * scale * gain_ref[...]).astype(jnp.bfloat16)
    kept = kept_ref.shape[1]
    kept_ref[...] = tokens_ref[:, pl.ds(pl.multiple_of(at_ref[0] * kept, 128), kept)]
    copies[1].wait()
    drive = jnp.dot(normed, w_in_ref[...], preferred_element_type=jnp.float32).astype(jnp.bfloat16)
    copies[2].wait()
    copies[3].wait()
    for half, skip_row in enumerate(skip_rows):
        cols = slice(half * block, (half + 1) * block)
        spans = slice(half * per_half * lanes, (half + 1) * per_half * lanes)
        part = drive[:, cols]
        driven = jnp.dot(part, in_ref[:, spans], preferred_element_type=jnp.float32)
        for place in range(per_half):
            g = half * per_half + place
            row = slice(g, g + 1)
            drive_re = driven[:, place * lanes : place * lanes + entries]
            drive_im = driven[:, place * lanes + entries : (place + 1) * lanes]
            old_re, old_im = state_re_ref[:, g, :], state_im_ref[:, g, :]
            push_re = coef_re[row] * drive_re - coef_im[row] * drive_im
            push_im = coef_re[row] * drive_im + coef_im[row] * drive_re
            new_re = turn_re[row] * old_re - turn_im[row] * old_im + push_re
            new_im = turn_re[row] * old_im + turn_im[row] * old_re + push_im
            new_re_ref[:, g, :] = new_re
            new_im_ref[:, g, :] = new_im
            both = jnp.concatenate([new_re, new_im], axis=1)
            high = both.astype(jnp.bfloat16)
            low = (both - high.astype(jnp.float32)).astype(jnp.bfloat16)
            split_ref[:seqs, g * lanes : (g + 1) * lanes] = high
            split_ref[seqs:, g * lanes : (g + 1) * lanes] = low
        terms = lax.dot_general(
            split_ref[:, spans],
            out_ref[:, spans],
            (((1,), (1,)), ((), ())),
            preferred_element_type=jnp.float32,
        )
        read = terms[:seqs] + terms[seqs:] + skip_row * part.astype(jnp.float32)
        mixed_ref[:, cols] = jax.nn.gelu(read).astype(jnp.bfloat16)


def front(
    at, tokens, mix_gain, w_in, decay_re, freq, log_step, in_re, in_im, out_re, out_im, skip,
    state_re, state_im, kept_width,
):
    groups, heads, entries = in_re.shape
    seqs = tokens.shape[0]
    per_half = min(groups, max(1, 128 // heads))
    vmem = pl.BlockSpec(memory_space=pltpu.VMEM)
    hbm = pl.BlockSpec(memory_space=pltpu.HBM)
    wide = (per_half * heads, groups * 2 * entries)
    return pl.pallas_call(
        mixer_front,
        out_shape=[
            pltpu.VMEM((seqs, groups * heads), jnp.bfloat16),
            pltpu.VMEM((seqs, kept_width), jnp.bfloat16),
            jax.ShapeDtypeStruct(state_re.shape, jnp.float32),
            jax.ShapeDtypeStruct(state_im.shape, jnp.float32),
        ],
        in_specs=[pl.BlockSpec(memory_space=pltpu.SMEM)] + [vmem] * 9 + [hbm] * 4,
        out_specs=[vmem] * 4,
        scratch_shapes=[
            pltpu.VMEM(tokens.shape, tokens.dtype),
            pltpu.VMEM(w_in.shape, w_in.dtype),
            pltpu.VMEM(state_re.shape, state_re.dtype),
            pltpu.VMEM(state_im.shape, state_im.dtype),
            pltpu.VMEM(wide, jnp.bfloat16),
            pltpu.VMEM(wide, jnp.bfloat16),
            pltpu.VMEM((2 * seqs, wide[1]), jnp.bfloat16),
            pltpu.SemaphoreType.DMA((4,)),
        ],
        compiler_params=pltpu.CompilerParams(vmem_limit_bytes=60 * 1024 * 1024),
        cost_estimate=pl.CostEstimate(
            flops=8_000_000_000, bytes_accessed=4_000_000, transcendentals=0
        ),
        name="mixer_front",
    )(
        at, mix_gain[None, :], log_step[None, :], decay_re, freq, in_re, in_im, out_re, out_im,
        skip, tokens, w_in, state_re, state_im,
    )


def fetch_weights(pieces, *refs):
    count = (len(refs) - 2) // 2
    sources, targets, sems = refs[1 : 1 + count], refs[1 + count : 1 + 2 * count], refs[-1]
    copies = []
    for source, target in zip(sources, targets):
        rows = source.shape[0] // pieces
        for piece in range(pieces):
            span = pl.ds(piece * rows, rows)
            copies.append(
                pltpu.make_async_copy(source.at[span], target.at[span], sems.at[len(copies)])
            )
    for copy in copies:
        copy.start()
    for copy in copies:
        copy.wait()


def fetched(after, *weights):
    pieces = 4
    return pl.pallas_call(
        functools.partial(fetch_weights, pieces),
        out_shape=[pltpu.VMEM(weight.shape, weight.dtype) for weight in weights],
        in_specs=[pl.BlockSpec(memory_space=pl.ANY)]
        + [pl.BlockSpec(memory_space=pltpu.HBM)] * len(weights),
        out_specs=[pl.BlockSpec(memory_space=pltpu.VMEM)] * len(weights),
        scratch_shapes=[pltpu.SemaphoreType.DMA((pieces * len(weights),))],
        compiler_params=pltpu.CompilerParams(vmem_limit_bytes=1024 * 1024),
        cost_estimate=pl.CostEstimate(
            flops=1_000_000_000, bytes_accessed=4_000_000 * len(weights), transcendentals=0
        ),
        name="fetch_weights",
    )(after, *(pltpu.with_memory_space_constraint(weight, pltpu.HBM) for weight in weights))


def expert_step(first, last, model_width, at_ref, block_ref, gain_ref, gate_ref, up_ref, *rest):
    held, results = (() if first else rest[:3]), (rest if first else rest[3:])
    width = block_ref.shape[1]
    start = pl.multiple_of(at_ref[0] * width, 128)
    values = block_ref[...].astype(jnp.float32)
    scaled = (values * gain_ref[:, pl.ds(start, width)]).astype(jnp.bfloat16)
    sums = lane_sums(values * values)
    gate = jnp.dot(scaled, gate_ref[pl.ds(start, width), :], preferred_element_type=jnp.float32)
    up = jnp.dot(scaled, up_ref[pl.ds(start, width), :], preferred_element_type=jnp.float32)
    if not first:
        gate, up, sums = gate + held[0][...], up + held[1][...], sums + held[2][...]
    if not last:
        results[0][...], results[1][...], results[2][...] = gate, up, sums
        return
    squares = jnp.sum(sums, axis=1, keepdims=True)
    scale = lax.rsqrt(squares / model_width + norm_eps)
    gate = gate * scale
    results[0][...] = (gate / (1.0 + jnp.exp(-gate)) * (up * scale)).astype(jnp.bfloat16)


def expert_part(block, at, gain, gate_w, up_w, held, last):
    rows, hidden_width = block.shape[0], gate_w.shape[1]
    model_width = gate_w.shape[0]
    if last:
        shapes = [jax.ShapeDtypeStruct((rows, hidden_width), jnp.bfloat16)]
    else:
        shapes = [
            jax.ShapeDtypeStruct((rows, hidden_width), jnp.float32),
            jax.ShapeDtypeStruct((rows, hidden_width), jnp.float32),
            jax.ShapeDtypeStruct((rows, 128), jnp.float32),
        ]
    vmem = pl.BlockSpec(memory_space=pltpu.VMEM)
    return pl.pallas_call(
        functools.partial(expert_step, not held, last, model_width),
        out_shape=shapes,
        in_specs=[pl.BlockSpec(memory_space=pltpu.SMEM)] + [vmem] * (4 + len(held)),
        out_specs=[vmem] * len(shapes),
        compiler_params=pltpu.CompilerParams(vmem_limit_bytes=24 * 1024 * 1024),
        cost_estimate=pl.CostEstimate(
            flops=4 * rows * block.shape[1] * hidden_width,
            bytes_accessed=4 * block.shape[1] * hidden_width,
            transcendentals=0,
        ),
        name="expert_last" if last else "expert_part",
    )(at, block, gain, gate_w, up_w, *held)


def local(
    tokens,
    mix_gain,
    w_in,
    decay_re,
    freq,
    log_step,
    in_re,
    in_im,
    out_re,
    out_im,
    skip,
    state_re,
    state_im,
    glu_weight,
    glu_bias,
    out_weight,
    ffn_gain,
    route,
    route_weight,
    expert_gate,
    expert_up,
    expert_down,
):
    seq_count = tokens.shape[0]
    groups_local = decay_re.shape[0]
    model_width = tokens.shape[1]
    shards = lax.axis_size("tp")
    local_width = model_width // shards
    experts = lax.axis_size("ep")
    top_count = route.shape[1]
    slot_cap = (3 * seq_count * top_count + 2 * experts - 1) // (2 * experts)
    rows_all = experts * slot_cap
    own = lax.axis_index("tp")
    offsets = list(range(1, shards))
    gate_local = expert_gate[0]
    up_local = expert_up[0]
    down_local = expert_down[0]

    def rows_of(array, offset, width):
        return lax.dynamic_slice_in_dim(array, (own ^ offset) * width, width, 0)

    def cols_of(array, offset, width):
        return lax.dynamic_slice_in_dim(array, (own ^ offset) * width, width, 1)

    own_at = own.astype(jnp.int32).reshape(1)
    mixed_in, token_part, new_re, new_im = front(
        own_at, tokens, mix_gain, w_in, decay_re, freq, log_step, in_re, in_im, out_re, out_im,
        skip, state_re, state_im, local_width,
    )
    chan_width = mixed_in.shape[1]

    arrived_mix = [partner_swap(mixed_in, offset) for offset in offsets]
    gate = jnp.dot(
        mixed_in, rows_of(glu_weight, 0, chan_width), preferred_element_type=jnp.float32
    )
    for offset, block in zip(offsets, arrived_mix):
        gate = gate + jnp.dot(
            block, rows_of(glu_weight, offset, chan_width), preferred_element_type=jnp.float32
        )
    gated = (mixed_in.astype(jnp.float32) * jax.nn.sigmoid(gate + glu_bias)).astype(jnp.bfloat16)

    (down_near,) = fetched(gated, down_local)

    def share(offset):
        block = jnp.dot(
            gated, cols_of(out_weight, offset, local_width), preferred_element_type=jnp.float32
        )
        return block.astype(jnp.bfloat16)

    arrived_shares = [partner_swap(share(offset), offset) for offset in offsets]
    mix_part = share(0).astype(jnp.float32)
    for block in arrived_shares:
        mix_part = mix_part + block.astype(jnp.float32)
    resid_part = (token_part.astype(jnp.float32) + mix_part).astype(
        jnp.bfloat16
    )

    flat_route = route.reshape(-1)
    hits = (flat_route[:, None] == jnp.arange(experts)[None, :]).astype(jnp.int32)
    rank = jnp.sum((jnp.cumsum(hits, axis=0) - hits) * hits, axis=1)
    relative = flat_route ^ lax.axis_index("ep")
    pairs = experts // 2
    slot = ((relative % 2) * pairs + relative // 2) * slot_cap + rank
    slot_ids = jnp.arange(rows_all)
    picks = (slot[None, :] == slot_ids[:, None]).reshape(rows_all, seq_count, top_count)
    select = jnp.any(picks, axis=2).astype(jnp.bfloat16)
    combine = jnp.einsum("ask,sk->sa", picks.astype(jnp.float32), route_weight)

    outbound = jnp.dot(select, resid_part, preferred_element_type=jnp.float32).astype(jnp.bfloat16)
    arrived, joined = to_experts(outbound.reshape(2, pairs, slot_cap, local_width))
    arrived = arrived.reshape(rows_all, local_width)
    gate_near, up_near = fetched(joined, gate_local, up_local)
    blocks = [(0, arrived)] + [(offset, partner_swap(arrived, offset)) for offset in offsets]
    held = ()
    for offset, block in blocks:
        at = (own ^ offset).astype(jnp.int32).reshape(1)
        held = expert_part(
            block, at, ffn_gain[None, :], gate_near, up_near, held, offset == shards - 1
        )
    hidden = held[0]

    def result(offset):
        block = jnp.dot(
            hidden, cols_of(down_near, offset, local_width), preferred_element_type=jnp.float32
        )
        return block.astype(jnp.bfloat16)

    arrived_results = [partner_swap(result(offset), offset) for offset in offsets]
    back_rows = result(0).astype(jnp.float32)
    for block in arrived_results:
        back_rows = back_rows + block.astype(jnp.float32)
    returned = from_experts(
        back_rows.astype(jnp.bfloat16).reshape(pairs, 2, slot_cap, local_width)
    ).reshape(rows_all, local_width)
    expert_total = lax.dot_general(
        combine,
        returned.astype(jnp.float32),
        (((1,), (0,)), ((), ())),
        precision=lax.Precision.HIGHEST,
    )
    mixed = (resid_part.astype(jnp.float32) + expert_total).astype(jnp.bfloat16)
    return (mixed, new_re, new_im)


def solution(mesh):
    in_specs = (
        P("ep", None),
        P(),
        P(None, "tp"),
        P("tp", None),
        P("tp", None),
        P("tp"),
        P("tp", None, None),
        P("tp", None, None),
        P("tp", None, None),
        P("tp", None, None),
        P("tp", None),
        P("ep", "tp", None),
        P("ep", "tp", None),
        P(None, "tp"),
        P("tp"),
        P("tp", None),
        P(),
        P("ep", None),
        P("ep", None),
        P("ep", None, "tp"),
        P("ep", None, "tp"),
        P("ep", "tp", None),
    )
    out_specs = (P("ep", "tp"), P("ep", "tp", None), P("ep", "tp", None))
    return jax.shard_map(local, mesh=mesh, in_specs=in_specs, out_specs=out_specs, check_vma=False)
```

```python
import functools

import jax
import jax.numpy as jnp
from jax import lax
from jax.experimental import pallas as pl
from jax.experimental.pallas import tpu as pltpu
from jax.sharding import PartitionSpec as P


norm_eps = 1e-06


def swap(value, axis, offset):
    pairs = [(source, source ^ offset) for source in range(lax.axis_size(axis))]
    return lax.ppermute(value, axis, pairs)


def near_first(count):
    return sorted(range(1, count), key=lambda offset: (offset.bit_count(), offset))


def far_first(count):
    return sorted(range(1, count), key=lambda offset: (-offset.bit_count(), offset))


def to_experts(rows):
    pairs = rows.shape[1]
    near = rows[0]
    crossed = swap(rows[1], "ep", 1)
    joined = jnp.stack([near, crossed], axis=1)
    moved = [None] + [swap(joined[step], "ep", 2 * step) for step in range(pairs - 1, 0, -1)][::-1]
    moved[0] = joined[0]
    return jnp.stack(moved, axis=0), joined


def from_experts(rows):
    pairs = rows.shape[0]
    moved = [None] + [swap(rows[step], "ep", 2 * step) for step in range(pairs - 1, 0, -1)][::-1]
    moved[0] = rows[0]
    moved = jnp.stack(moved, axis=1)
    return moved[0], swap(moved[1], "ep", 1)


def lane_sums(values):
    total = values[:, :128]
    for start in range(128, values.shape[1], 128):
        total = total + values[:, start : start + 128]
    return total


def mixer_front(
    at_ref, *refs
):
    count = 13
    sources, (mixed_ref, kept_ref, new_re_ref, new_im_ref) = refs[:count], refs[count : count + 4]
    targets = refs[count + 4 : 2 * count + 4]
    in_ref, out_ref, split_ref, sems = refs[2 * count + 4 :]
    copies = [
        pltpu.make_async_copy(source, target, sems.at[place])
        for place, (source, target) in enumerate(zip(sources, targets))
    ]
    for copy in copies:
        copy.start()
    (
        tokens_ref, gain_ref, in_re_ref, in_im_ref, log_step_ref, decay_ref, freq_ref, w_in_ref,
        state_re_ref, state_im_ref, out_re_ref, out_im_ref, skip_ref,
    ) = targets
    groups, heads, entries = in_re_ref.shape
    seqs, width = tokens_ref.shape
    per_half = min(groups, max(1, 128 // heads))
    lanes = 2 * entries
    in_ref[...] = jnp.zeros_like(in_ref)
    out_ref[...] = jnp.zeros_like(out_ref)
    copies[0].wait()
    copies[1].wait()
    values = tokens_ref[...].astype(jnp.float32)
    squares = jnp.sum(lane_sums(values * values), axis=1, keepdims=True)
    scale = lax.rsqrt(squares / width + norm_eps)
    normed = (values * scale * gain_ref[...]).astype(jnp.bfloat16)
    kept = kept_ref.shape[1]
    kept_ref[...] = tokens_ref[:, pl.ds(pl.multiple_of(at_ref[0] * kept, 128), kept)]

    copies[2].wait()
    copies[3].wait()
    for g in range(groups):
        rows = pl.ds((g % per_half) * heads, heads)
        in_ref[rows, g * lanes : (g + 1) * lanes] = jnp.concatenate(
            [in_re_ref[g], in_im_ref[g]], axis=1
        )
    for copy in copies[4:7]:
        copy.wait()

    diagonal = lax.broadcasted_iota(jnp.int32, (groups, groups), 0) == lax.broadcasted_iota(
        jnp.int32, (groups, groups), 1
    )
    step = jnp.sum(
        jnp.where(diagonal, jnp.exp(log_step_ref[...]), 0.0), axis=1, keepdims=True
    )
    decay, freq = decay_ref[...], freq_ref[...]
    magnitude = jnp.exp(decay * step)
    turn_re = magnitude * jnp.cos(freq * step)
    turn_im = magnitude * jnp.sin(freq * step)
    denom = decay * decay + freq * freq
    coef_re = ((turn_re - 1.0) * decay + turn_im * freq) / denom
    coef_im = (turn_im * decay - (turn_re - 1.0) * freq) / denom

    copies[7].wait()
    drive = jnp.dot(normed, w_in_ref[...], preferred_element_type=jnp.float32).astype(jnp.bfloat16)
    for copy in copies[8:]:
        copy.wait()
    for g in range(groups):
        rows = pl.ds((g % per_half) * heads, heads)
        out_ref[rows, g * lanes : (g + 1) * lanes] = jnp.concatenate(
            [out_re_ref[g], -out_im_ref[g]], axis=1
        )
    block = per_half * heads
    skip_tiled = jnp.concatenate([skip_ref[...]] * per_half, axis=1)
    owner = lax.broadcasted_iota(jnp.int32, skip_tiled.shape, 1) // heads
    group = lax.broadcasted_iota(jnp.int32, skip_tiled.shape, 0)
    skip_rows = [
        jnp.sum(jnp.where(owner + start == group, skip_tiled, 0.0), axis=0, keepdims=True)
        for start in range(0, groups, per_half)
    ]

    for half, skip_row in enumerate(skip_rows):
        cols = slice(half * block, (half + 1) * block)
        spans = slice(half * per_half * lanes, (half + 1) * per_half * lanes)
        part = drive[:, cols]
        driven = jnp.dot(part, in_ref[:, spans], preferred_element_type=jnp.float32)
        for place in range(per_half):
            g = half * per_half + place
            row = slice(g, g + 1)
            drive_re = driven[:, place * lanes : place * lanes + entries]
            drive_im = driven[:, place * lanes + entries : (place + 1) * lanes]
            old_re, old_im = state_re_ref[:, g, :], state_im_ref[:, g, :]
            push_re = coef_re[row] * drive_re - coef_im[row] * drive_im
            push_im = coef_re[row] * drive_im + coef_im[row] * drive_re
            new_re = turn_re[row] * old_re - turn_im[row] * old_im + push_re
            new_im = turn_re[row] * old_im + turn_im[row] * old_re + push_im
            new_re_ref[:, g, :] = new_re
            new_im_ref[:, g, :] = new_im
            both = jnp.concatenate([new_re, new_im], axis=1)
            high = both.astype(jnp.bfloat16)
            low = (both - high.astype(jnp.float32)).astype(jnp.bfloat16)
            split_ref[:seqs, g * lanes : (g + 1) * lanes] = high
            split_ref[seqs:, g * lanes : (g + 1) * lanes] = low
        terms = lax.dot_general(
            split_ref[:, spans],
            out_ref[:, spans],
            (((1,), (1,)), ((), ())),
            preferred_element_type=jnp.float32,
        )
        read = terms[:seqs] + terms[seqs:] + skip_row * part.astype(jnp.float32)
        mixed_ref[:, cols] = jax.nn.gelu(read).astype(jnp.bfloat16)


def front(
    at, tokens, mix_gain, w_in, decay_re, freq, log_step, in_re, in_im, out_re, out_im, skip,
    state_re, state_im, kept_width,
):
    groups, heads, entries = in_re.shape
    seqs = tokens.shape[0]
    per_half = min(groups, max(1, 128 // heads))
    inputs = (
        tokens, mix_gain[None, :], in_re, in_im, log_step[None, :], decay_re, freq, w_in,
        state_re, state_im, out_re, out_im, skip,
    )
    vmem = pl.BlockSpec(memory_space=pltpu.VMEM)
    hbm = pl.BlockSpec(memory_space=pltpu.HBM)
    wide = (per_half * heads, groups * 2 * entries)
    return pl.pallas_call(
        mixer_front,
        out_shape=[
            pltpu.VMEM((seqs, groups * heads), jnp.bfloat16),
            pltpu.VMEM((seqs, kept_width), jnp.bfloat16),
            pltpu.VMEM(state_re.shape, jnp.float32),
            pltpu.VMEM(state_im.shape, jnp.float32),
        ],
        in_specs=[pl.BlockSpec(memory_space=pltpu.SMEM)] + [hbm] * len(inputs),
        out_specs=[vmem] * 4,
        scratch_shapes=[
            *(pltpu.VMEM(value.shape, value.dtype) for value in inputs),
            pltpu.VMEM(wide, jnp.bfloat16),
            pltpu.VMEM(wide, jnp.bfloat16),
            pltpu.VMEM((2 * seqs, wide[1]), jnp.bfloat16),
            pltpu.SemaphoreType.DMA((len(inputs),)),
        ],
        compiler_params=pltpu.CompilerParams(vmem_limit_bytes=12 * 1024 * 1024),
        cost_estimate=pl.CostEstimate(
            flops=8_000_000_000, bytes_accessed=4_000_000, transcendentals=0
        ),
        name="mixer_front",
    )(at, *(pltpu.with_memory_space_constraint(value, pltpu.HBM) for value in inputs))


def move_arrays(pieces, *refs):
    count = (len(refs) - 2) // 2
    sources, targets, sems = refs[1 : 1 + count], refs[1 + count : 1 + 2 * count], refs[-1]
    copies = []
    for source, target in zip(sources, targets):
        rows = source.shape[0] // pieces
        for piece in range(pieces):
            span = pl.ds(piece * rows, rows)
            copies.append(
                pltpu.make_async_copy(source.at[span], target.at[span], sems.at[len(copies)])
            )
    for copy in copies:
        copy.start()
    for copy in copies:
        copy.wait()


def moved(after, fetches, stores=()):
    pieces = 4
    count = len(fetches) + len(stores)
    hbm, vmem = pl.BlockSpec(memory_space=pltpu.HBM), pl.BlockSpec(memory_space=pltpu.VMEM)
    return pl.pallas_call(
        functools.partial(move_arrays, pieces),
        out_shape=[pltpu.VMEM(value.shape, value.dtype) for value in fetches]
        + [pltpu.HBM(value.shape, value.dtype) for value in stores],
        in_specs=[pl.BlockSpec(memory_space=pl.ANY)] + [hbm] * len(fetches) + [vmem] * len(stores),
        out_specs=[vmem] * len(fetches) + [hbm] * len(stores),
        scratch_shapes=[pltpu.SemaphoreType.DMA((pieces * count,))],
        compiler_params=pltpu.CompilerParams(vmem_limit_bytes=1024 * 1024),
        cost_estimate=pl.CostEstimate(
            flops=1_000_000_000, bytes_accessed=4_000_000 * count, transcendentals=0
        ),
        name="move_arrays",
    )(
        after,
        *(pltpu.with_memory_space_constraint(value, pltpu.HBM) for value in fetches),
        *stores,
    )


def expert_step(first, last, model_width, at_ref, block_ref, gain_ref, gate_ref, up_ref, *rest):
    held, results = (() if first else rest[:3]), (rest if first else rest[3:])
    width = block_ref.shape[1]
    start = pl.multiple_of(at_ref[0] * width, 128)
    values = block_ref[...].astype(jnp.float32)
    scaled = (values * gain_ref[:, pl.ds(start, width)]).astype(jnp.bfloat16)
    sums = lane_sums(values * values)
    gate = jnp.dot(scaled, gate_ref[pl.ds(start, width), :], preferred_element_type=jnp.float32)
    up = jnp.dot(scaled, up_ref[pl.ds(start, width), :], preferred_element_type=jnp.float32)
    if not first:
        gate, up, sums = gate + held[0][...], up + held[1][...], sums + held[2][...]
    if not last:
        results[0][...], results[1][...], results[2][...] = gate, up, sums
        return
    squares = jnp.sum(sums, axis=1, keepdims=True)
    scale = lax.rsqrt(squares / model_width + norm_eps)
    gate = gate * scale
    results[0][...] = (gate / (1.0 + jnp.exp(-gate)) * (up * scale)).astype(jnp.bfloat16)


def expert_part(block, at, gain, gate_w, up_w, held, last):
    rows, hidden_width = block.shape[0], gate_w.shape[1]
    model_width = gate_w.shape[0]
    if last:
        shapes = [jax.ShapeDtypeStruct((rows, hidden_width), jnp.bfloat16)]
    else:
        shapes = [
            jax.ShapeDtypeStruct((rows, hidden_width), jnp.float32),
            jax.ShapeDtypeStruct((rows, hidden_width), jnp.float32),
            jax.ShapeDtypeStruct((rows, 128), jnp.float32),
        ]
    vmem = pl.BlockSpec(memory_space=pltpu.VMEM)
    return pl.pallas_call(
        functools.partial(expert_step, not held, last, model_width),
        out_shape=shapes,
        in_specs=[pl.BlockSpec(memory_space=pltpu.SMEM)] + [vmem] * (4 + len(held)),
        out_specs=[vmem] * len(shapes),
        compiler_params=pltpu.CompilerParams(vmem_limit_bytes=24 * 1024 * 1024),
        cost_estimate=pl.CostEstimate(
            flops=4 * rows * block.shape[1] * hidden_width,
            bytes_accessed=4 * block.shape[1] * hidden_width,
            transcendentals=0,
        ),
        name="expert_last" if last else "expert_part",
    )(at, block, gain, gate_w, up_w, *held)


def local(
    tokens,
    mix_gain,
    w_in,
    decay_re,
    freq,
    log_step,
    in_re,
    in_im,
    out_re,
    out_im,
    skip,
    state_re,
    state_im,
    glu_weight,
    glu_bias,
    out_weight,
    ffn_gain,
    route,
    route_weight,
    expert_gate,
    expert_up,
    expert_down,
):
    seq_count = tokens.shape[0]
    model_width = tokens.shape[1]
    shards = lax.axis_size("tp")
    local_width = model_width // shards
    experts = lax.axis_size("ep")
    top_count = route.shape[1]
    slot_cap = (3 * seq_count * top_count + 2 * experts - 1) // (2 * experts)
    rows_all = experts * slot_cap
    own = lax.axis_index("tp")
    offsets = near_first(shards)
    gate_local = expert_gate[0]
    up_local = expert_up[0]
    down_local = expert_down[0]

    def rows_of(array, offset, width):
        return lax.dynamic_slice_in_dim(array, (own ^ offset) * width, width, 0)

    def cols_of(array, offset, width):
        return lax.dynamic_slice_in_dim(array, (own ^ offset) * width, width, 1)

    own_at = own.astype(jnp.int32).reshape(1)
    mixed_in, token_part, new_re, new_im = front(
        own_at, tokens, mix_gain, w_in, decay_re, freq, log_step, in_re, in_im, out_re, out_im,
        skip, state_re, state_im, local_width,
    )
    chan_width = mixed_in.shape[1]

    arrived_mix = [swap(mixed_in, "tp", offset) for offset in offsets]
    gate = jnp.dot(
        mixed_in, rows_of(glu_weight, 0, chan_width), preferred_element_type=jnp.float32
    )
    for offset, block in zip(offsets, arrived_mix):
        gate = gate + jnp.dot(
            block, rows_of(glu_weight, offset, chan_width), preferred_element_type=jnp.float32
        )
    gated = (mixed_in.astype(jnp.float32) * jax.nn.sigmoid(gate + glu_bias)).astype(jnp.bfloat16)

    down_near, new_re, new_im = moved(gated, (down_local,), (new_re, new_im))

    def share(offset):
        block = jnp.dot(
            gated, cols_of(out_weight, offset, local_width), preferred_element_type=jnp.float32
        )
        return block.astype(jnp.bfloat16)

    arrived_shares = []
    for offset in far_first(shards):
        block = share(offset)
        arrived_shares.append(swap(block, "tp", offset))
    mix_part = share(0).astype(jnp.float32)
    for block in arrived_shares:
        mix_part = mix_part + block.astype(jnp.float32)
    resid_part = (token_part.astype(jnp.float32) + mix_part).astype(
        jnp.bfloat16
    )

    flat_route = route.reshape(-1)
    hits = (flat_route[:, None] == jnp.arange(experts)[None, :]).astype(jnp.int32)
    rank = jnp.sum((jnp.cumsum(hits, axis=0) - hits) * hits, axis=1)
    relative = flat_route ^ lax.axis_index("ep")
    pairs = experts // 2
    slot = ((relative % 2) * pairs + relative // 2) * slot_cap + rank
    slot_ids = jnp.arange(rows_all)
    picks = (slot[None, :] == slot_ids[:, None]).reshape(rows_all, seq_count, top_count)
    select = jnp.any(picks, axis=2).astype(jnp.bfloat16)
    combine = jnp.einsum("ask,sk->sa", picks.astype(jnp.float32), route_weight)

    outbound = jnp.dot(select, resid_part, preferred_element_type=jnp.float32).astype(jnp.bfloat16)
    arrived, joined = to_experts(outbound.reshape(2, pairs, slot_cap, local_width))
    arrived = arrived.reshape(rows_all, local_width)
    gate_near, up_near = moved(joined, (gate_local, up_local))
    blocks = [(0, arrived)] + [(offset, swap(arrived, "tp", offset)) for offset in offsets]
    held = ()
    for place, (offset, block) in enumerate(blocks):
        at = (own ^ offset).astype(jnp.int32).reshape(1)
        held = expert_part(
            block, at, ffn_gain[None, :], gate_near, up_near, held, place == shards - 1
        )
    hidden = held[0]

    def result(offset):
        block = jnp.dot(
            hidden, cols_of(down_near, offset, local_width), preferred_element_type=jnp.float32
        )
        return block.astype(jnp.bfloat16)

    arrived_results = []
    for offset in offsets:
        block = result(offset)
        arrived_results.append(swap(block, "tp", offset))
    kept_result = lax.optimization_barrier(result(0))
    back_rows = kept_result.astype(jnp.float32)
    for block in arrived_results:
        back_rows = back_rows + block.astype(jnp.float32)
    near, crossed = from_experts(
        back_rows.astype(jnp.bfloat16).reshape(pairs, 2, slot_cap, local_width)
    )
    half = rows_all // 2

    def weighed(rows, start):
        return lax.dot_general(
            combine[:, start : start + half],
            rows.reshape(half, local_width).astype(jnp.float32),
            (((1,), (0,)), ((), ())),
            precision=lax.Precision.HIGHEST,
        )

    total = lax.optimization_barrier(resid_part.astype(jnp.float32) + weighed(near, 0))
    mixed = (total + weighed(crossed, half)).astype(jnp.bfloat16)
    return (mixed, new_re, new_im)


def solution(mesh):
    in_specs = (
        P("ep", None),
        P(),
        P(None, "tp"),
        P("tp", None),
        P("tp", None),
        P("tp"),
        P("tp", None, None),
        P("tp", None, None),
        P("tp", None, None),
        P("tp", None, None),
        P("tp", None),
        P("ep", "tp", None),
        P("ep", "tp", None),
        P(None, "tp"),
        P("tp"),
        P("tp", None),
        P(),
        P("ep", None),
        P("ep", None),
        P("ep", None, "tp"),
        P("ep", None, "tp"),
        P("ep", "tp", None),
    )
    out_specs = (P("ep", "tp"), P("ep", "tp", None), P("ep", "tp", None))
    return jax.shard_map(local, mesh=mesh, in_specs=in_specs, out_specs=out_specs, check_vma=False)
```
